32 devices in a mesh: fs: 8 (over z, x), tp: 4 (over y, core).
Axes of the slice: x: 2, y: 2, z: 4, core: 2. Of those that a mesh axis runs over, the one named last changes fastest.
Arguments:
- tokens: bfloat16 [3072, 4096], P('fs', 'tp'), may hold values from -600 to 600
- gate_master: float32 [8, 4096, 512], P(None, 'fs', 'tp'), may hold values from -0.09375 to 0.09375
- up_master: float32 [8, 4096, 512], P(None, 'fs', 'tp'), may hold values from -0.09375 to 0.09375
- down_master: float32 [8, 4096, 512], P(None, 'fs', 'tp'), may hold values from -0.25 to 0.25
- norm_gain: float32 [4096], P('fs'), may hold values from 0.1 to 1.9
- routes: int32 [3072, 2], P('fs'), may hold values from 0 to 7, all different within a row; in each aligned block of 384 rows (0 to 383, 384 to 767, ...) at most 192 rows name the same one
- route_weight: float32 [3072, 2], P('fs'), may hold values from 0.1 to 1
Outputs:
- gate_out: bfloat16 [8, 4096, 512], P('fs', None, 'tp')
- up_out: bfloat16 [8, 4096, 512], P('fs', None, 'tp')
- down_out: bfloat16 [8, 4096, 512], P('fs', None, 'tp')
- mixed: bfloat16 [3072, 4096], P('fs', 'tp')
The draws below stay inside these ranges and needn't reach their ends.
Inputs may be any that keep to these rules, and one draw needn't show every extreme that they name: `routes`: within the rows of one index of fs no expert is named by more than 192 pairs, a bound that some block reaches; the 2 experts of a row differ.
All inputs are finite; a program needn't handle non-finite values.
Results may differ from the reference program's by a relative error of at most 0.0087.
Values may be sent and summed in bfloat16 or wider, within the bound.
No kernel may reach another device: no remote copies, remote signals or barrier semaphores. Data moves between devices by JAX's collectives and lax.ppermute only.
A program may use at most 128 MiB of HBM per device.

```python
import math
import jax
import jax.numpy as jnp
import numpy as np
from jax import lax

D = 4096
FF = 512
TOP = 2
TOK_DEV = 384
EXPERTS = 8
TOKENS = 3072
CAP = 192
N_FS = 8


def draw_tokens(key, part):
    k_base, k_rows, k_cols = jax.random.split(key, 3)
    row_scale = jnp.exp(jax.random.uniform(k_rows, (TOKENS, 1), jnp.float32) * math.log(10.0))
    position = jnp.arange(D, dtype=jnp.float32)[None, :] / D
    col_scale = jnp.exp(position * math.log(3.0) + jax.random.uniform(k_cols, (1, D), jnp.float32) * math.log(3.3))
    base = jnp.clip(jax.random.normal(k_base, (TOKENS, D), jnp.float32), -6.0, 6.0)
    return (base * row_scale * col_scale).astype(jnp.bfloat16)


def shard_levels(own_key, extent, cuts, low, high):
    def one(dim, shards_of):
        steps = jax.random.uniform(jax.random.fold_in(jax.random.fold_in(own_key, 6), dim), (shards_of,), jnp.float32, low / len(cuts), high / len(cuts))
        return jnp.repeat(jnp.exp(steps), extent[dim] // shards_of).reshape((-1,) + (1,) * (len(extent) - dim - 1))

    factor_of = one(*cuts[0])
    for cut in cuts[1:]:
        factor_of = factor_of * one(*cut)
    return factor_of


def assign_block(own_key, own, number, rows, amount, top, most, slope):
    ranking = jax.random.permutation(own_key, amount)
    packed, ordinary = load_shares(amount, rows * top, most, slope, True), load_shares(amount, rows * top, most, slope, False)
    places = jnp.arange(amount)

    def named(sizes, rotation):
        used = int((sizes > 0).sum())
        fixed = max(1, used // 4)
        passed = fixed + (places - fixed + rotation * (used - fixed)) % max(1, amount - fixed)
        return jnp.zeros((amount,), jnp.int32).at[ranking[jnp.where(places < fixed, places, passed)]].set(jnp.asarray(sizes, jnp.int32))

    sizes = jnp.where(number % 4 == 0, named(packed, number // 4), named(ordinary, number - number // 4 - 1))
    mixed = jax.random.permutation(jax.random.fold_in(own, 3), amount)
    giver, taker = mixed[0:amount // 2 * 2:2], mixed[1:amount // 2 * 2:2]
    room = jnp.minimum(sizes[giver] - 1, most - sizes[taker]) // 2
    room = jnp.where((giver == ranking[0]) | (taker == ranking[0]) | (sizes[taker] == 0), 0, jnp.maximum(room, 0))
    passed = jax.random.randint(jax.random.fold_in(own, 4), (amount // 2,), 0, 1 << 20) % (room + 1)
    sizes = sizes.at[giver].add(-passed).at[taker].add(passed)
    members = jnp.searchsorted(jnp.cumsum(sizes), jnp.arange(rows * top), side="right").astype(jnp.int32)
    grid = members.reshape(top, rows).T
    grid = grid[jax.random.permutation(jax.random.fold_in(own, 1), rows)]
    rotation = jax.random.randint(jax.random.fold_in(own, 2), (rows, 1), 0, top)
    return jnp.take_along_axis(grid, (jnp.arange(top)[None, :] + rotation) % top, axis=1)


def load_shares(number_of, total, reach, skew, full):
    portions = [(1 << 20) // math.isqrt(rank ** skew) + 1 for rank in range(1, number_of + 1)]
    largest = reach if full else min(reach, max(-(-total // number_of), total * portions[0] // sum(portions)))
    least = 1 if total - largest >= number_of - 1 else 0
    holding, surplus = [largest] + [least] * (number_of - 1), total - largest - least * (number_of - 1)
    while surplus > 0:
        free = [i for i in range(1, number_of) if holding[i] < largest] or [i for i in range(1, number_of) if holding[i] < reach]
        pool, remaining = sum([portions[i] for i in free]), surplus
        for i in free:
            addition = min(reach - holding[i], max(1, remaining * portions[i] // pool), surplus)
            holding[i] = holding[i] + addition
            surplus = surplus - addition
    return np.array(holding)


def bell_draw(key, extent, width, bound, shards=(), kind=jnp.bfloat16):
    values = jax.random.normal(key, extent, jnp.float32) * width
    if len(shards) > 0:
        values = shard_levels(key, extent, shards, -0.22, 0.18) * values
    return jnp.clip(values, min=-bound, max=bound).astype(kind)


def setup_inputs(seed: int = 0) -> dict:
    keys = jax.random.split(jax.random.key(seed), 8)
    tokens = draw_tokens(jax.random.fold_in(keys[7], 71), 0)
    gate_master = bell_draw(keys[1], (EXPERTS, D, FF), D ** -0.5, 0.09375, ((1, 8), (2, 4)), jnp.float32)
    up_master = bell_draw(keys[2], (EXPERTS, D, FF), D ** -0.5, 0.09375, ((1, 8), (2, 4)), jnp.float32)
    down_master = bell_draw(keys[3], (EXPERTS, D, FF), FF ** -0.5, 0.25, ((1, 8), (2, 4)), jnp.float32)
    norm_gain = jnp.clip(1.0 + 0.18 * jax.random.normal(keys[4], (D,), jnp.float32), 0.1, 1.9)
    routes_keys = jax.random.split(jax.random.fold_in(keys[5], 1), TOKENS // TOK_DEV)
    routes_turns = jax.random.permutation(jax.random.fold_in(keys[5], 3), TOKENS // TOK_DEV)
    routes = jax.vmap(lambda own, number: assign_block(jax.random.fold_in(keys[5], 2), own, number, TOK_DEV, EXPERTS, TOP, CAP, 2))(routes_keys, routes_turns).reshape((TOKENS, TOP))
    route_weight = jnp.clip(jnp.exp(math.log(1.0) - 2.3025851 * jax.random.uniform(keys[6], (TOKENS, TOP), jnp.float32) ** shard_levels(keys[6], (TOKENS, TOP), ((0, 8),), -0.2, 0.2)), 0.1, 1.0)
    return dict(tokens=tokens, gate_master=gate_master, up_master=up_master, down_master=down_master, norm_gain=norm_gain, routes=routes, route_weight=route_weight)


norm_eps = 1e-06

def slot_table(expert_ids, n_experts, capacity, top_count):
    assigned = expert_ids.shape[0]
    onehot = (expert_ids[:, None] == jnp.arange(n_experts, dtype=jnp.int32)[None, :]).astype(jnp.int32)
    before = jnp.cumsum(onehot, axis=0) - onehot
    slots = lax.optimization_barrier(jnp.sum(before * onehot, axis=1)).astype(jnp.int32)
    position = expert_ids * capacity + slots
    owners = jnp.arange(assigned, dtype=jnp.int32) // top_count
    matches = position[None, :] == jnp.arange(n_experts * capacity, dtype=jnp.int32)[:, None]
    slot_token = lax.optimization_barrier(jnp.max(jnp.where(matches, owners[None, :], -1), axis=1)).astype(jnp.int32)
    return (slots, slot_token)

def reference(tokens, gate_master, up_master, down_master, norm_gain, routes, route_weight):
    folded = norm_gain[None, :, None]
    gate_out = (gate_master * folded).astype(jnp.bfloat16)
    up_out = (up_master * folded).astype(jnp.bfloat16)
    down_out = down_master.astype(jnp.bfloat16)
    token_float = tokens.astype(jnp.float32)
    inverse = lax.rsqrt(lax.optimization_barrier(jnp.mean(token_float * token_float, axis=1, keepdims=True)) + norm_eps)
    normed = (token_float * inverse).astype(jnp.bfloat16)
    mix_weights = route_weight / lax.optimization_barrier(jnp.sum(route_weight, axis=1, keepdims=True))
    block_routes = routes.reshape(N_FS, TOK_DEV * TOP)

    def per_block(one_block):
        return slot_table(one_block, EXPERTS, CAP, TOP)
    slots, slot_token = jax.vmap(per_block)(block_routes)
    offsets = jnp.arange(N_FS, dtype=jnp.int32)[:, None] * TOK_DEV
    global_token = jnp.where(slot_token < 0, TOKENS, slot_token + offsets).astype(jnp.int32)
    padded = jnp.concatenate([normed, jnp.zeros((1, D), jnp.bfloat16)], axis=0)

    def run_expert(expert):
        columns = lax.dynamic_slice_in_dim(global_token, expert * CAP, CAP, 1).reshape(-1)
        expert_rows = padded[columns]
        gate_mat = lax.dynamic_index_in_dim(gate_out, expert, 0, keepdims=False)
        up_mat = lax.dynamic_index_in_dim(up_out, expert, 0, keepdims=False)
        down_mat = lax.dynamic_index_in_dim(down_out, expert, 0, keepdims=False)
        gate_val = jnp.dot(expert_rows, gate_mat, preferred_element_type=jnp.float32)
        up_val = jnp.dot(expert_rows, up_mat, preferred_element_type=jnp.float32)
        hidden = (jax.nn.silu(gate_val) * up_val).astype(jnp.bfloat16)
        result = lax.dot_general(hidden, down_mat, (((1,), (1,)), ((), ())), preferred_element_type=jnp.float32)
        return result.astype(jnp.bfloat16)
    outputs = lax.map(run_expert, jnp.arange(EXPERTS, dtype=jnp.int32))
    flat_out = outputs.reshape(-1, D)
    block_index = jnp.arange(N_FS, dtype=jnp.int32)[:, None]
    index = ((block_routes * N_FS + block_index) * CAP + slots).astype(jnp.int32)
    gathered = flat_out[index.reshape(-1)].astype(jnp.float32).reshape(TOKENS, TOP, D)
    mixed = lax.optimization_barrier(jnp.sum(mix_weights[:, :, None] * gathered, axis=1)).astype(jnp.bfloat16)
    return (gate_out, up_out, down_out, mixed)
```

```python
import jax
import jax.numpy as jnp
from jax import lax
from jax.experimental import pallas as pl
from jax.experimental.pallas import tpu as pltpu
from jax.sharding import PartitionSpec as P

norm_eps = 1e-06
f32 = jnp.float32
bf16 = jnp.bfloat16


def bits_of(n):
    return n.bit_length() - 1


def swap(x, axis, j):
    n = lax.axis_size(axis)
    return lax.ppermute(x, axis, [(s, s ^ j) for s in range(n)])


def reversed_bits(p, n_bits):
    return sum(((p >> k) & 1) << (n_bits - 1 - k) for k in range(n_bits))


def in_kernel(body, out, *args, flops=0):
    nbytes = sum(a.size * a.dtype.itemsize for a in args)
    return pl.pallas_call(
        body,
        out_shape=out,
        in_specs=[pl.BlockSpec(memory_space=pltpu.VMEM)] * len(args),
        out_specs=pl.BlockSpec(memory_space=pltpu.VMEM),
        cost_estimate=pl.CostEstimate(flops=flops, bytes_accessed=nbytes, transcendentals=0),
    )(*args)


def tile_of(rows, most=192):
    t = most
    while rows % t:
        t //= 2
    return t


def up_kernel(r_ref, x_ref, g_ref, u_ref, o_ref):
    rows = x_ref.shape[0]
    n_experts, _, ff = g_ref.shape
    t = tile_of(rows)

    def tile(i, _):
        at = pl.ds(pl.multiple_of(i * t, t), t)
        x = x_ref[at, :]
        first, second = r_ref[at, 0:1], r_ref[at, 1:2]

        def step(e, sums):
            w = jnp.concatenate([g_ref[e], u_ref[e]], axis=1)
            p = jnp.dot(x, w, preferred_element_type=f32)
            return jnp.where(first == e, p, sums[0]), jnp.where(second == e, p, sums[1])

        zero = jnp.zeros((t, 2 * ff), f32)
        a, b = lax.fori_loop(0, n_experts, step, (zero, zero), unroll=n_experts <= 8)
        o_ref[at, : 2 * ff] = a.astype(bf16)
        o_ref[at, 2 * ff :] = b.astype(bf16)
        return 0

    lax.fori_loop(0, rows // t, tile, 0)


def down_kernel(r_ref, h_ref, d_ref, o_ref):
    rows = h_ref.shape[0]
    n_experts, ff, width = d_ref.shape
    t = tile_of(rows)
    zero = jnp.zeros((t, ff), bf16)

    def tile(i, _):
        at = pl.ds(pl.multiple_of(i * t, t), t)
        h = h_ref[at, :]
        first, second = r_ref[at, 0:1], r_ref[at, 1:2]

        def piece(e):
            return jnp.where(first == e, h[:, :ff], jnp.where(second == e, h[:, ff:], zero))

        def step(e, acc):
            pair = jnp.concatenate([piece(2 * e), piece(2 * e + 1)], axis=1)
            w = jnp.concatenate([d_ref[2 * e], d_ref[2 * e + 1]], axis=0)
            return acc + jnp.dot(pair, w, preferred_element_type=f32)

        acc = lax.fori_loop(
            0, n_experts // 2, step, jnp.zeros((t, width), f32), unroll=n_experts <= 8
        )
        o_ref[at, :] = acc.astype(o_ref.dtype)
        return 0

    lax.fori_loop(0, rows // t, tile, 0)


def body(tokens, gate_master, up_master, down_master, norm_gain, routes, route_weight):
    n_fs, n_tp = lax.axis_size("fs"), lax.axis_size("tp")
    i, t = lax.axis_index("fs"), lax.axis_index("tp")
    n_bits = bits_of(n_fs)
    lo = n_fs // n_tp
    n_experts, w, ff = gate_master.shape
    rows, top = routes.shape
    group = rows // n_tp
    place = [reversed_bits(p, n_bits) for p in range(n_fs)]

    folded = norm_gain[None, :, None]
    gate_cast = (gate_master * folded).astype(bf16)
    up_cast = (up_master * folded).astype(bf16)
    down_cast = down_master.astype(bf16)
    down_turned = jnp.swapaxes(down_cast, 1, 2)

    sliced = tokens.reshape(n_tp, group, lo, w).transpose(0, 2, 1, 3)
    mine = [lax.dynamic_index_in_dim(sliced, t ^ j, 0, keepdims=False) for j in range(n_tp)]
    quarters = jnp.stack([mine[0]] + [swap(mine[j], "tp", j) for j in range(1, n_tp)])
    quarters = quarters.reshape(n_fs, group, w)
    base = t * lo

    def slice_for(j):
        s = (i ^ j) ^ base
        return lax.dynamic_index_in_dim(quarters, s, 0, keepdims=False)

    own = [slice_for(j) if j == 0 else swap(slice_for(j), "fs", j) for j in place]
    own = jnp.concatenate(own, axis=0)

    chunks = {0: own}
    have = [0]
    for k in reversed(range(bits_of(n_tp))):
        for g in list(have):
            chunks[g | (1 << k)] = swap(chunks[g], "tp", 1 << k)
        have = have + [g | (1 << k) for g in have]

    def by_group(a):
        a = a.reshape((n_tp, group) + a.shape[1:])
        return [lax.dynamic_index_in_dim(a, t ^ g, 0, keepdims=False) for g in range(n_tp)]

    route_groups = jnp.stack(by_group(routes)).transpose(0, 2, 1).reshape(1, n_tp, top * group)
    for k in reversed(range(n_bits)):
        route_groups = jnp.concatenate([route_groups, swap(route_groups, "fs", 1 << k)], axis=0)
    route_groups = route_groups.reshape(n_fs, n_tp, top, group).transpose(1, 0, 3, 2)
    route_groups = route_groups.reshape(n_tp, n_fs * group, top)

    token_float = tokens.astype(f32)
    full_width = w * n_fs
    sumsquares = jnp.sum(token_float * token_float, axis=1)
    for k in range(bits_of(n_tp)):
        sumsquares = sumsquares + swap(sumsquares, "tp", 1 << k)
    inverse = by_group(lax.rsqrt(sumsquares / full_width + norm_eps)[:, None])
    mix = by_group(route_weight / jnp.sum(route_weight, axis=1, keepdims=True))

    order = [0] + sorted(range(2, n_tp), key=lambda g: g) + ([1] if n_tp > 1 else [])
    half = n_fs * group // 2
    up_flops = 4 * half * w * n_experts * ff
    outs = {}
    for g in order:
        r, x = route_groups[g], chunks[g]
        shape = jax.ShapeDtypeStruct((half, 4 * ff), bf16)
        send = in_kernel(up_kernel, shape, r[half:], x[half:], gate_cast, up_cast, flops=up_flops)
        keep = in_kernel(up_kernel, shape, r[:half], x[:half], gate_cast, up_cast, flops=up_flops)
        for k in range(n_bits):
            total = keep.astype(f32) + swap(send, "fs", 1 << k).astype(f32)
            if k < n_bits - 1:
                m = total.shape[0] // 2
                total = total.astype(bf16)
                keep, send = total[:m], total[m:]
        total = total * inverse[g]
        hidden = []
        for k in range(top):
            v = total[:, 2 * k * ff : (2 * k + 1) * ff]
            u = total[:, (2 * k + 1) * ff : (2 * k + 2) * ff]
            hidden.append((jax.nn.silu(v) * u * mix[g][:, k : k + 1]).astype(bf16))
        hidden = jnp.concatenate(hidden, axis=1)
        for k in reversed(range(n_bits)):
            hidden = jnp.concatenate([hidden, swap(hidden, "fs", 1 << k)], axis=0)
        outs[g] = in_kernel(
            down_kernel,
            jax.ShapeDtypeStruct((n_fs * group, w), bf16),
            r,
            hidden,
            down_turned,
            flops=2 * n_fs * group * w * n_experts * ff,
        )

    live = n_tp
    for k in range(bits_of(n_tp)):
        bit = 1 << k
        for g in [g for g in sorted(outs) if g & bit]:
            got = swap(outs.pop(g), "tp", bit)
            outs[g ^ bit] = (outs[g ^ bit].astype(f32) + got.astype(f32)).astype(bf16)
    final = outs[0].reshape(n_fs, group, w)
    home = jnp.stack([final[p] if j == 0 else swap(final[p], "fs", j) for p, j in enumerate(place)])
    by_j = jnp.stack([home[place.index(j)] for j in range(n_fs)])
    mixed = jnp.zeros((n_tp, group, lo * w), bf16)
    for r in range(n_tp):
        parts = [
            lax.dynamic_index_in_dim(by_j, i ^ ((t ^ r) * lo + l), 0, keepdims=False)
            for l in range(lo)
        ]
        part = jnp.concatenate(parts, axis=1)
        if r:
            part = swap(part, "tp", r)
        mixed = lax.dynamic_update_index_in_dim(mixed, part, t ^ r, 0)
    mixed = mixed.reshape(rows, lo * w)

    gate_out, up_out, down_out = (
        lax.all_to_all(a, "fs", split_axis=0, concat_axis=1, tiled=True)
        for a in (gate_cast, up_cast, down_cast)
    )
    return (gate_out, up_out, down_out, mixed)


def solution(mesh):
    placed = (
        P("fs", "tp"),
        P(None, "fs", "tp"),
        P(None, "fs", "tp"),
        P(None, "fs", "tp"),
        P("fs"),
        P("fs", None),
        P("fs", None),
    )
    return jax.shard_map(
        body,
        mesh=mesh,
        in_specs=placed,
        out_specs=(P("fs", None, "tp"), P("fs", None, "tp"), P("fs", None, "tp"), P("fs", "tp")),
        check_vma=False,
    )
```
